32 devices in a mesh: ra: 8 (over z, y), cb: 4 (over x, core).
Axes of the slice: x: 2, y: 2, z: 4, core: 2. Of those that a mesh axis runs over, the one named last changes fastest.
Arguments:
- tokens: bfloat16 [512, 4096], P(None, 'ra'), may hold values from -4 to 4, as said below
- pre_gain_first: float32 [4096], P('ra'), may hold values from 0.1 to 1.9
- gate_first: bfloat16 [4096, 11264], P('ra', 'cb'), may hold values from -0.125 to 0.125
- up_first: bfloat16 [4096, 11264], P('ra', 'cb'), may hold values from -0.125 to 0.125
- down_first: bfloat16 [11264, 4096], P('cb', 'ra'), may hold values from -0.078125 to 0.078125
- post_gain_first: float32 [4096], P('ra'), may hold values from 0.1 to 1.9
- pre_gain_second: float32 [4096], P('ra'), may hold values from 0.1 to 1.9
- gate_second: bfloat16 [4096, 11264], P('ra', 'cb'), may hold values from -0.125 to 0.125
- up_second: bfloat16 [4096, 11264], P('ra', 'cb'), may hold values from -0.125 to 0.125
- down_second: bfloat16 [11264, 4096], P('cb', 'ra'), may hold values from -0.078125 to 0.078125
- post_gain_second: float32 [4096], P('ra'), may hold values from 0.1 to 1.9
Outputs:
- mixed: bfloat16 [512, 4096], P(None, 'ra')
The draws below stay inside these ranges and needn't reach their ends.
Inputs may be any that keep to these rules, and one draw needn't show every extreme that they name: `tokens`: each block of 128 consecutive channels has its own scale, and rows have their own scales.
All inputs are finite; a program needn't handle non-finite values.
Results may differ from the reference program's by a relative error of at most 0.0071.
Values may be sent and summed in bfloat16 or wider, within the bound.
A program may use at most 64 MiB of HBM per device.

```python
import jax
import jax.numpy as jnp
from jax import lax

D = 4096
FF = 11264
TOKENS = 512


def draw_tokens(key, part):
    base_key = jax.random.fold_in(key, 11)
    key_noise, key_block, key_row, key_common = jax.random.split(base_key, 4)
    noise = jax.random.normal(key_noise, (TOKENS, D), jnp.float32)
    block_scale = jnp.exp(jax.random.uniform(key_block, (32,), jnp.float32, jnp.log(0.15), jnp.log(0.6)))
    column_scale = jnp.repeat(block_scale, D // 32)
    row_scale = jax.random.uniform(key_row, (TOKENS, 1), jnp.float32, 0.7, 1.4)
    values = noise * column_scale[None, :] * row_scale
    return jnp.clip(values, -4.0, 4.0).astype(jnp.bfloat16)


def spiked(drawn, key, source, target, parts, factor):
    owner, partner = [(jnp.arange(drawn.shape[dim]) // (drawn.shape[dim] // parts)).reshape([-1 if axis == dim else 1 for axis in range(drawn.ndim)]) for dim in (source, target)]
    chosen = jax.random.permutation(key, parts)[partner]
    strong = (owner == chosen) | (owner == (partner + parts // 2) % parts)
    return jnp.where(strong, factor * drawn, drawn)


def level_of(own_key, shape, cuts, low, top_value):
    factor_of = 1.0
    for position, blocks in cuts:
        heights = jax.random.uniform(jax.random.fold_in(jax.random.fold_in(own_key, 6), position), (blocks,), jnp.float32, low / len(cuts), top_value / len(cuts))
        factor_of = factor_of * jnp.repeat(jnp.exp(heights), shape[position] // blocks).reshape((-1,) + (1,) * (len(shape) - 1 - position))
    return factor_of


def gaussian_with(key, dims, spread, bound, cuts, heavy, kind=jnp.bfloat16):
    result = spread * jax.random.normal(key, dims, jnp.float32)
    if cuts:
        result = result * level_of(key, dims, cuts, -0.22, 0.18)
    return jnp.clip(spiked(result, jax.random.fold_in(key, 3), *heavy), -bound, bound).astype(kind)


def setup_inputs(seed: int = 0) -> dict:
    arg_keys = jax.random.split(jax.random.key(seed), 12)
    tokens = draw_tokens(jax.random.fold_in(arg_keys[11], 71), 0)
    pre_gain_first = jnp.clip(1.0 + 0.18 * jax.random.normal(arg_keys[1], (D,), jnp.float32), 0.1, 1.9)
    gate_first = gaussian_with(arg_keys[2], (D, FF), D ** -0.5, 0.125, ((0, 8), (1, 4)), (0, 1, 8, 2.0))
    up_first = gaussian_with(arg_keys[3], (D, FF), D ** -0.5, 0.125, ((0, 8), (1, 4)), (0, 1, 8, 2.0))
    down_first = gaussian_with(arg_keys[4], (FF, D), FF ** -0.5, 0.078125, ((0, 4), (1, 8)), (0, 1, 8, 2.0))
    post_gain_first = jnp.clip(1.0 + 0.18 * jax.random.normal(arg_keys[5], (D,), jnp.float32), 0.1, 1.9)
    pre_gain_second = jnp.clip(1.0 + 0.18 * jax.random.normal(arg_keys[6], (D,), jnp.float32), 0.1, 1.9)
    gate_second = gaussian_with(arg_keys[7], (D, FF), D ** -0.5, 0.125, ((0, 8), (1, 4)), (0, 1, 8, 2.0))
    up_second = gaussian_with(arg_keys[8], (D, FF), D ** -0.5, 0.125, ((0, 8), (1, 4)), (0, 1, 8, 2.0))
    down_second = gaussian_with(arg_keys[9], (FF, D), FF ** -0.5, 0.078125, ((0, 4), (1, 8)), (0, 1, 8, 2.0))
    post_gain_second = jnp.clip(1.0 + 0.18 * jax.random.normal(arg_keys[10], (D,), jnp.float32), 0.1, 1.9)
    return dict(tokens=tokens, pre_gain_first=pre_gain_first, gate_first=gate_first, up_first=up_first, down_first=down_first, post_gain_first=post_gain_first, pre_gain_second=pre_gain_second, gate_second=gate_second, up_second=up_second, down_second=down_second, post_gain_second=post_gain_second)


EPS = 1e-06

def row_scale(values):
    return lax.rsqrt(lax.optimization_barrier(jnp.mean(values * values, axis=-1, keepdims=True)) + EPS)

def half_step(resid, pre_gain, gate_weight, up_weight, down_weight, post_gain):
    normed = (resid * row_scale(resid) * pre_gain).astype(jnp.bfloat16)
    gate_value = jnp.dot(normed, gate_weight, preferred_element_type=jnp.float32)
    up_value = jnp.dot(normed, up_weight, preferred_element_type=jnp.float32)
    hidden = (jax.nn.silu(gate_value) * up_value).astype(jnp.bfloat16)
    branch = jnp.dot(hidden, down_weight, preferred_element_type=jnp.float32)
    return resid + 0.5 * branch * row_scale(branch) * post_gain

def reference(tokens, pre_gain_first, gate_first, up_first, down_first, post_gain_first, pre_gain_second, gate_second, up_second, down_second, post_gain_second):
    resid = tokens.astype(jnp.float32)
    middle = half_step(resid, pre_gain_first, gate_first, up_first, down_first, post_gain_first)
    final = half_step(middle, pre_gain_second, gate_second, up_second, down_second, post_gain_second)
    return final.astype(jnp.bfloat16)
```

```python
import functools

import jax
import jax.numpy as jnp
from jax import lax
from jax.experimental import pallas as pl
from jax.experimental.pallas import tpu as pltpu
from jax.sharding import PartitionSpec as P

EPS = 1e-06
MESH = pl.DeviceIdType.MESH
F32 = jnp.float32
BF16 = jnp.bfloat16


def log2(n):
    return n.bit_length() - 1


def bits_of(index, count):
    return [lax.rem(index // (1 << b), 2) for b in range(count)]


def spread(col, lanes):
    return jnp.broadcast_to(col, (col.shape[0], 128)).T[0:8]


def column(row):
    return jnp.broadcast_to(row[0:1], (128, row.shape[1])).T


def half_step(
    first, n, nc, width, *refs
):
    k, kc = log2(n), log2(nc)
    (h_ref, resid_ref, ss_ref, post_ref, pre_ref, gate_hbm, up_hbm, down_hbm), refs = refs[:8], refs[8:]
    if first:
        (h_out, mid_out, ss_out), refs = refs[:3], refs[3:]
    else:
        (y_out,), refs = refs[:1], refs[1:]
    (gate_v, up_v, down_v, acc, hid, branch, scale, ss_slots, br_slots, br_send, ag, ss_all), refs = refs[:12], refs[12:]
    snd, refs = refs[:k], refs[k:]
    rcv, refs = refs[:k], refs[k:]
    csnd, refs = refs[:kc], refs[kc:]
    crcv, refs = refs[:kc], refs[kc:]
    (w_sem, rs_s, rs_r, ag_s, ag_r, c_s, c_r, ss_s, ss_r, br_s, br_r, cg_s, cg_r, cs_s, cs_r) = refs

    tokens, depth = h_ref.shape
    chunks, _, cw = gate_v.shape
    me, col = lax.axis_index("ra"), lax.axis_index("cb")
    eb, xb = bits_of(me, k), bits_of(col, kc)
    partners = [me + (1 - 2 * eb[b]) * (1 << b) for b in range(k)]
    cpartners = [col + (1 - 2 * xb[b]) * (1 << b) for b in range(kc)]
    crows = tokens // nc

    def weights(c):
        cols = pl.ds(pl.multiple_of(c * cw, 128), cw)
        return [
            pltpu.make_async_copy(gate_hbm.at[:, cols], gate_v.at[c], w_sem.at[0, c]),
            pltpu.make_async_copy(up_hbm.at[:, cols], up_v.at[c], w_sem.at[1, c]),
            pltpu.make_async_copy(down_hbm.at[cols, :], down_v.at[c], w_sem.at[2, c]),
        ]

    @pl.loop(0, chunks)
    def _(c):
        for copy in weights(c):
            copy.start()

    barrier = pltpu.get_barrier_semaphore()

    def xor(index, bits, off):
        out = index
        for b, bit in enumerate(bits):
            if (off >> b) & 1:
                out = out + (1 - 2 * bit) * (1 << b)
        return out

    for off in range(1, n):
        pl.semaphore_signal(barrier, inc=1, device_id={"ra": xor(me, eb, off)}, device_id_type=MESH)
    for off in range(1, nc):
        pl.semaphore_signal(barrier, inc=1, device_id={"cb": xor(col, xb, off)}, device_id_type=MESH)
    pl.semaphore_wait(barrier, n - 1 + nc - 1)

    def remote(src, dst, s, r, **where):
        return pltpu.make_async_remote_copy(
            src_ref=src, dst_ref=dst, send_sem=s, recv_sem=r, device_id=where, device_id_type=MESH
        )

    def ss_copy(off):
        return remote(ss_ref, ss_slots.at[off - 1], ss_s.at[off - 1], ss_r.at[off - 1], ra=xor(me, eb, off))

    for off in range(1, n):
        ss_copy(off).start()

    def plan(c):
        swap = jnp.where(lax.rem(c, 4) == 1, 1, 0)
        bits, to = list(eb), list(partners)
        if k > 1:
            bits[0], bits[1] = eb[0] + swap * (eb[1] - eb[0]), eb[1] + swap * (eb[0] - eb[1])
            to[0] = partners[0] + swap * (partners[1] - partners[0])
            to[1] = partners[1] + swap * (partners[0] - partners[1])
        return bits, to

    def rows_at(base, size):
        return pl.ds(pl.multiple_of(base, size), size)

    def rs_copy(c, s, to):
        return remote(snd[s].at[c], rcv[s].at[c], rs_s.at[s, c], rs_r.at[s, c], ra=to[s])

    def ag_copy(c, s, bits, to):
        size = tokens >> (s + 1)
        base = sum(bits[i] * (tokens >> (i + 1)) for i in range(s + 1))
        part = hid.at[c, rows_at(base, size), :]
        return remote(part, part, ag_s.at[s, c], ag_r.at[s, c], ra=to[s])

    branch[...] = jnp.zeros_like(branch)

    def tick(t, carry):
        @pl.when(t < chunks)
        def _():
            c = t
            bits, to = plan(c)
            gate_copy, up_copy, _ = weights(c)
            gate_copy.wait()
            up_copy.wait()
            half = tokens // 2
            theirs = h_ref[rows_at((1 - bits[0]) * half, half), :]
            snd[0][c, :, :cw] = jnp.dot(theirs, gate_v[c], preferred_element_type=F32).astype(BF16)
            snd[0][c, :, cw:] = jnp.dot(theirs, up_v[c], preferred_element_type=F32).astype(BF16)
            rs_copy(c, 0, to).start()
            mine = h_ref[rows_at(bits[0] * half, half), :]
            acc[c, :, :cw] = jnp.dot(mine, gate_v[c], preferred_element_type=F32)
            acc[c, :, cw:] = jnp.dot(mine, up_v[c], preferred_element_type=F32)

        for s in range(1, k):
            @pl.when((t >= s) & (t < chunks + s))
            def _():
                c = t - s
                bits, to = plan(c)
                rs_copy(c, s - 1, to).wait()
                size = tokens >> (s + 1)
                base = sum(bits[i] * (tokens >> (i + 1)) for i in range(1, s))
                out = (1 - bits[s]) * size
                snd[s][c] = (
                    acc[c, rows_at(base + out, size), :] + rcv[s - 1][c, rows_at(out, size), :].astype(F32)
                ).astype(BF16)
                rs_copy(c, s, to).start()
                keep = bits[s] * size
                acc[c, rows_at(base + keep, size), :] += rcv[s - 1][c, rows_at(keep, size), :].astype(F32)

        @pl.when(t == k)
        def _():
            for off in range(1, n):
                ss_copy(off).wait()
            total = ss_ref[...]
            for off in range(1, n):
                total = total + ss_slots[off - 1]
            for b in range(nc):
                scale[b * crows : (b + 1) * crows, :] = column(lax.rsqrt(total[b] / width + EPS))

        @pl.when((t >= k) & (t < chunks + k))
        def _():
            c = t - k
            bits, to = plan(c)
            rs_copy(c, k - 1, to).wait()
            size = tokens >> k
            base = sum(bits[i] * (tokens >> (i + 1)) for i in range(1, k))
            value = acc[c, rows_at(base, size), :] + rcv[k - 1][c].astype(F32)
            rows = rows_at(base + bits[0] * (tokens // 2), size)
            factor = scale[rows, 0:1]
            g, u = value[:, :cw] * factor, value[:, cw:] * factor
            hid[c, rows, :] = (g / (1.0 + jnp.exp(-g)) * u).astype(BF16)
            ag_copy(c, k - 1, bits, to).start()

        for s in range(k - 1, 0, -1):
            lag = 2 * k - s
            @pl.when((t >= lag) & (t < chunks + lag))
            def _():
                c = t - lag
                bits, to = plan(c)
                ag_copy(c, s, bits, to).wait()
                ag_copy(c, s - 1, bits, to).start()

        @pl.when(t >= 2 * k)
        def _():
            c = t - 2 * k
            bits, to = plan(c)
            ag_copy(c, 0, bits, to).wait()
            weights(c)[2].wait()
            branch[...] += jnp.dot(hid[c], down_v[c], preferred_element_type=F32)

        return carry

    lax.fori_loop(0, chunks + 2 * k, tick, 0)

    def c_copy(s):
        return remote(csnd[s], crcv[s], c_s.at[s], c_r.at[s], cb=cpartners[s])

    base = 0
    for s in range(kc):
        size = tokens >> (s + 1)
        out, keep = (1 - xb[s]) * size, xb[s] * size
        mine = branch[rows_at(base + out, size), :]
        if s:
            mine = mine + crcv[s - 1][rows_at(out, size), :].astype(F32)
        csnd[s][...] = mine.astype(csnd[s].dtype)
        c_copy(s).start()
        if s:
            branch[rows_at(base + keep, size), :] += crcv[s - 1][rows_at(keep, size), :].astype(F32)
        c_copy(s).wait()
        base = base + keep
    own = rows_at(base, crows)
    total = branch[own, :] + crcv[kc - 1][...].astype(F32)

    br_send[...] = spread(jnp.sum(total * total, axis=1, keepdims=True), crows)

    def br_copy(off):
        return remote(br_send, br_slots.at[off - 1], br_s.at[off - 1], br_r.at[off - 1], ra=xor(me, eb, off))

    for off in range(1, n):
        br_copy(off).start()
    squares = br_send[...]
    for off in range(1, n):
        br_copy(off).wait()
        squares = squares + br_slots[off - 1]
    factor = column(0.5 * lax.rsqrt(squares / width + EPS))[:, 0:1]
    resid = resid_ref[own, :].astype(F32) if first else resid_ref[...]
    middle = resid + factor * total * post_ref[...]
    if first:
        ag[own, :] = (middle * pre_ref[...]).astype(BF16)
        mid_out[...] = middle
    else:
        ag[own, :] = middle.astype(BF16)

    bases = [0]
    for s in range(kc):
        bases.append(bases[-1] + xb[s] * (tokens >> (s + 1)))

    def cg_copy(s):
        part = ag.at[rows_at(bases[s + 1], tokens >> (s + 1)), :]
        return remote(part, part, cg_s.at[s], cg_r.at[s], cb=cpartners[s])

    cg_copy(kc - 1).start()
    if first:
        block = sum(xb[s] * (nc >> (s + 1)) for s in range(kc))
        ss_all[block] = spread(jnp.sum(middle * middle, axis=1, keepdims=True), crows)

        def cs_copy(off):
            part = ss_all.at[block]
            return remote(part, part, cs_s.at[off - 1], cs_r.at[off - 1], cb=xor(col, xb, off))

        for off in range(1, nc):
            cs_copy(off).start()
    for s in range(kc - 1, -1, -1):
        cg_copy(s).wait()
        if s:
            cg_copy(s - 1).start()
    if first:
        for off in range(1, nc):
            cs_copy(off).wait()
        ss_out[...] = ss_all[...]
        h_out[...] = ag[...]
    else:
        y_out[...] = ag[...]


def run(first, n, nc, width, h, resid, ss, post, pre, gate, up, down):
    tokens, depth = h.shape
    hidden = gate.shape[1]
    cw = 256 if hidden % 256 == 0 else 128
    chunks = hidden // cw
    k, kc, crows = log2(n), log2(nc), tokens // nc
    vmem = pl.BlockSpec(memory_space=pltpu.VMEM)
    hbm = pl.BlockSpec(memory_space=pl.ANY)
    dma = pltpu.SemaphoreType.DMA
    if first:
        out = [
            jax.ShapeDtypeStruct((tokens, depth), BF16),
            jax.ShapeDtypeStruct((crows, depth), F32),
            jax.ShapeDtypeStruct((nc, 8, crows), F32),
        ]
    else:
        out = [jax.ShapeDtypeStruct((tokens, depth), BF16)]
    scratch = [
        pltpu.VMEM((chunks, depth, cw), BF16),
        pltpu.VMEM((chunks, depth, cw), BF16),
        pltpu.VMEM((chunks, cw, depth), BF16),
        pltpu.VMEM((chunks, tokens // 2, 2 * cw), F32),
        pltpu.VMEM((chunks, tokens, cw), BF16),
        pltpu.VMEM((tokens, depth), F32),
        pltpu.VMEM((tokens, 128), F32),
        pltpu.VMEM((n - 1, nc, 8, crows), F32),
        pltpu.VMEM((n - 1, 8, crows), F32),
        pltpu.VMEM((8, crows), F32),
        pltpu.VMEM((tokens, depth), BF16),
        pltpu.VMEM((nc, 8, crows), F32),
    ]
    scratch += [pltpu.VMEM((chunks, tokens >> (s + 1), 2 * cw), BF16) for s in range(k)] * 2
    scratch += [pltpu.VMEM((tokens >> (s + 1), depth), BF16 if s else F32) for s in range(kc)] * 2
    scratch += [dma((3, chunks))] + [dma((k, chunks))] * 4 + [dma((kc,))] * 2
    scratch += [dma((n - 1,))] * 4 + [dma((kc,))] * 2 + [dma((nc - 1,))] * 2
    return pl.pallas_call(
        functools.partial(half_step, first, n, nc, width),
        out_shape=out,
        in_specs=[vmem] * 5 + [hbm] * 3,
        out_specs=[vmem] * len(out),
        scratch_shapes=scratch,
        compiler_params=pltpu.CompilerParams(
            collective_id=0 if first else 1, has_side_effects=True, vmem_limit_bytes=60 * 1024 * 1024
        ),
        name="first" if first else "second",
    )(h, resid, ss, post, pre, gate, up, down)


def solution(mesh):
    n, nc = mesh.shape["ra"], mesh.shape["cb"]

    def body(tokens, pre1, gate1, up1, down1, post1, pre2, gate2, up2, down2, post2):
        count, depth = tokens.shape
        width = depth * n
        resid = tokens.astype(F32)
        squares = jnp.sum(resid * resid, axis=1).reshape(nc, 1, count // nc)
        ss = jnp.broadcast_to(squares, (nc, 8, count // nc))
        h = (resid * pre1[None, :]).astype(BF16)
        row = lambda gain: gain.reshape(1, depth)
        h2, mid, ss2 = run(True, n, nc, width, h, tokens, ss, row(post1), row(pre2), gate1, up1, down1)
        (out,) = run(False, n, nc, width, h2, mid, ss2, row(post2), row(pre2), gate2, up2, down2)
        return out

    in_specs = (
        P(None, "ra"), P("ra"), P("ra", "cb"), P("ra", "cb"), P("cb", "ra"), P("ra"),
        P("ra"), P("ra", "cb"), P("ra", "cb"), P("cb", "ra"), P("ra"),
    )
    return jax.shard_map(body, mesh=mesh, in_specs=in_specs, out_specs=P(None, "ra"), check_vma=False)
```

```python
import functools

import jax
import jax.numpy as jnp
from jax import lax
from jax.experimental import pallas as pl
from jax.experimental.pallas import tpu as pltpu
from jax.sharding import PartitionSpec as P

EPS = 1e-06
MESH = pl.DeviceIdType.MESH
F32 = jnp.float32
BF16 = jnp.bfloat16


def log2(n):
    return n.bit_length() - 1


def bits_of(index, count):
    return [lax.rem(index // (1 << b), 2) for b in range(count)]


def spread(col, lanes):
    return jnp.broadcast_to(col, (col.shape[0], 128)).T[0:8]


def column(row):
    return jnp.broadcast_to(row[0:1], (128, row.shape[1])).T


def half_step(
    first, n, nc, width, *refs
):
    k, kc = log2(n), log2(nc)
    (h_ref, resid_ref, ss_ref, post_ref, pre_ref, gate_hbm, up_hbm, down_hbm), refs = refs[:8], refs[8:]
    if first:
        (h_out, mid_out, ss_out), refs = refs[:3], refs[3:]
    else:
        (y_out,), refs = refs[:1], refs[1:]
    (both_v, down_v, acc, hid, branch, scale, ss_slots, br_slots, br_send, ag, ss_all), refs = refs[:11], refs[11:]
    snd, refs = refs[:k], refs[k:]
    rcv, refs = refs[:k], refs[k:]
    csnd, refs = refs[:kc], refs[kc:]
    crcv, refs = refs[:kc], refs[kc:]
    (w_sem, rs_s, rs_r, ag_s, ag_r, c_s, c_r, ss_s, ss_r, br_s, br_r, cg_s, cg_r, cs_s, cs_r) = refs

    tokens, depth = h_ref.shape
    chunks, cw, _ = down_v.shape
    me, col = lax.axis_index("ra"), lax.axis_index("cb")
    eb, xb = bits_of(me, k), bits_of(col, kc)
    partners = [me + (1 - 2 * eb[b]) * (1 << b) for b in range(k)]
    cpartners = [col + (1 - 2 * xb[b]) * (1 << b) for b in range(kc)]
    crows = tokens // nc

    def weights(c):
        cols = pl.ds(pl.multiple_of(c * cw, 128), cw)
        return [
            pltpu.make_async_copy(gate_hbm.at[:, cols], both_v.at[c, :, pl.ds(0, cw)], w_sem.at[0, c]),
            pltpu.make_async_copy(up_hbm.at[:, cols], both_v.at[c, :, pl.ds(cw, cw)], w_sem.at[1, c]),
            pltpu.make_async_copy(down_hbm.at[cols, :], down_v.at[c], w_sem.at[2, c]),
        ]

    @pl.loop(0, chunks)
    def _(c):
        for copy in weights(c):
            copy.start()

    barrier = pltpu.get_barrier_semaphore()

    def xor(index, bits, off):
        out = index
        for b, bit in enumerate(bits):
            if (off >> b) & 1:
                out = out + (1 - 2 * bit) * (1 << b)
        return out

    for off in range(1, n):
        pl.semaphore_signal(barrier, inc=1, device_id={"ra": xor(me, eb, off)}, device_id_type=MESH)
    for off in range(1, nc):
        pl.semaphore_signal(barrier, inc=1, device_id={"cb": xor(col, xb, off)}, device_id_type=MESH)
    pl.semaphore_wait(barrier, n - 1 + nc - 1)

    def remote(src, dst, s, r, **where):
        return pltpu.make_async_remote_copy(
            src_ref=src, dst_ref=dst, send_sem=s, recv_sem=r, device_id=where, device_id_type=MESH
        )

    def ss_copy(off):
        return remote(ss_ref, ss_slots.at[off - 1], ss_s.at[off - 1], ss_r.at[off - 1], ra=xor(me, eb, off))

    for off in range(1, n):
        ss_copy(off).start()

    def plan(c):
        swap = jnp.where(lax.rem(c, 3) == 1, 1, 0)
        bits, to = list(eb), list(partners)
        if k > 1:
            bits[0], bits[1] = eb[0] + swap * (eb[1] - eb[0]), eb[1] + swap * (eb[0] - eb[1])
            to[0] = partners[0] + swap * (partners[1] - partners[0])
            to[1] = partners[1] + swap * (partners[0] - partners[1])
        return bits, to

    def rows_at(base, size):
        return pl.ds(pl.multiple_of(base, size), size)

    def rs_copy(c, s, to):
        return remote(snd[s].at[c], rcv[s].at[c], rs_s.at[s, c], rs_r.at[s, c], ra=to[s])

    def ag_copy(c, s, bits, to):
        size = tokens >> (s + 1)
        base = sum(bits[i] * (tokens >> (i + 1)) for i in range(s + 1))
        part = hid.at[c, rows_at(base, size), :]
        return remote(part, part, ag_s.at[s, c], ag_r.at[s, c], ra=to[s])

    branch[...] = jnp.zeros_like(branch)

    lags = [2 * i for i in range(2 * k + 1)]

    def tick(t, carry):
        @pl.when(t < chunks)
        def _():
            c = t
            bits, to = plan(c)
            gate_copy, up_copy, _ = weights(c)
            gate_copy.wait()
            up_copy.wait()
            half = tokens // 2
            theirs = h_ref[rows_at((1 - bits[0]) * half, half), :]
            snd[0][c] = jnp.dot(theirs, both_v[c], preferred_element_type=F32).astype(BF16)
            rs_copy(c, 0, to).start()
            mine = h_ref[rows_at(bits[0] * half, half), :]
            acc[c] = jnp.dot(mine, both_v[c], preferred_element_type=F32)

        for s in range(1, k):
            rs_lag = lags[s]
            @pl.when((t >= rs_lag) & (t < chunks + rs_lag))
            def _():
                c = t - rs_lag
                bits, to = plan(c)
                rs_copy(c, s - 1, to).wait()
                size = tokens >> (s + 1)
                base = sum(bits[i] * (tokens >> (i + 1)) for i in range(1, s))
                out = (1 - bits[s]) * size
                snd[s][c] = (
                    acc[c, rows_at(base + out, size), :] + rcv[s - 1][c, rows_at(out, size), :].astype(F32)
                ).astype(BF16)
                rs_copy(c, s, to).start()
                keep = bits[s] * size
                acc[c, rows_at(base + keep, size), :] += rcv[s - 1][c, rows_at(keep, size), :].astype(F32)

        @pl.when(t == lags[k])
        def _():
            for off in range(1, n):
                ss_copy(off).wait()
            total = ss_ref[...]
            for off in range(1, n):
                total = total + ss_slots[off - 1]
            for b in range(nc):
                scale[b * crows : (b + 1) * crows, :] = column(lax.rsqrt(total[b] / width + EPS))

        @pl.when((t >= lags[k]) & (t < chunks + lags[k]))
        def _():
            c = t - lags[k]
            bits, to = plan(c)
            rs_copy(c, k - 1, to).wait()
            size = tokens >> k
            base = sum(bits[i] * (tokens >> (i + 1)) for i in range(1, k))
            value = acc[c, rows_at(base, size), :] + rcv[k - 1][c].astype(F32)
            rows = rows_at(base + bits[0] * (tokens // 2), size)
            factor = scale[rows, 0:1]
            g, u = value[:, :cw] * factor, value[:, cw:] * factor
            hid[c, rows, :] = (g / (1.0 + jnp.exp(-g)) * u).astype(BF16)
            ag_copy(c, k - 1, bits, to).start()

        for s in range(k - 1, 0, -1):
            lag = lags[2 * k - s]
            @pl.when((t >= lag) & (t < chunks + lag))
            def _():
                c = t - lag
                bits, to = plan(c)
                ag_copy(c, s, bits, to).wait()
                ag_copy(c, s - 1, bits, to).start()

        @pl.when(t >= lags[2 * k])
        def _():
            c = t - lags[2 * k]
            bits, to = plan(c)
            ag_copy(c, 0, bits, to).wait()
            weights(c)[2].wait()
            branch[...] += jnp.dot(hid[c], down_v[c], preferred_element_type=F32)

        return carry

    lax.fori_loop(0, chunks + lags[2 * k], tick, 0)

    def c_copy(s):
        return remote(csnd[s], crcv[s], c_s.at[s], c_r.at[s], cb=cpartners[s])

    base = 0
    for s in range(kc):
        size = tokens >> (s + 1)
        out, keep = (1 - xb[s]) * size, xb[s] * size
        mine = branch[rows_at(base + out, size), :]
        if s:
            mine = mine + crcv[s - 1][rows_at(out, size), :].astype(F32)
        csnd[s][...] = mine.astype(csnd[s].dtype)
        c_copy(s).start()
        if s:
            branch[rows_at(base + keep, size), :] += crcv[s - 1][rows_at(keep, size), :].astype(F32)
        c_copy(s).wait()
        base = base + keep
    own = rows_at(base, crows)
    total = branch[own, :] + crcv[kc - 1][...].astype(F32)

    br_send[...] = spread(jnp.sum(total * total, axis=1, keepdims=True), crows)

    def br_copy(off):
        return remote(br_send, br_slots.at[off - 1], br_s.at[off - 1], br_r.at[off - 1], ra=xor(me, eb, off))

    for off in range(1, n):
        br_copy(off).start()
    squares = br_send[...]
    for off in range(1, n):
        br_copy(off).wait()
        squares = squares + br_slots[off - 1]
    factor = column(0.5 * lax.rsqrt(squares / width + EPS))[:, 0:1]
    resid = resid_ref[own, :].astype(F32) if first else resid_ref[...]
    middle = resid + factor * total * post_ref[...]
    if first:
        ag[own, :] = (middle * pre_ref[...]).astype(BF16)
        mid_out[...] = middle
    else:
        ag[own, :] = middle.astype(BF16)

    bases = [0]
    for s in range(kc):
        bases.append(bases[-1] + xb[s] * (tokens >> (s + 1)))

    def cg_copy(s):
        part = ag.at[rows_at(bases[s + 1], tokens >> (s + 1)), :]
        return remote(part, part, cg_s.at[s], cg_r.at[s], cb=cpartners[s])

    cg_copy(kc - 1).start()
    if first:
        block = sum(xb[s] * (nc >> (s + 1)) for s in range(kc))
        ss_all[block] = spread(jnp.sum(middle * middle, axis=1, keepdims=True), crows)

        def cs_copy(off):
            part = ss_all.at[block]
            return remote(part, part, cs_s.at[off - 1], cs_r.at[off - 1], cb=xor(col, xb, off))

        for off in range(1, nc):
            cs_copy(off).start()
    for s in range(kc - 1, -1, -1):
        cg_copy(s).wait()
        if s:
            cg_copy(s - 1).start()
    if first:
        for off in range(1, nc):
            cs_copy(off).wait()
        ss_out[...] = ss_all[...]
        h_out[...] = ag[...]
    else:
        y_out[...] = ag[...]


def run(first, n, nc, width, h, resid, ss, post, pre, gate, up, down):
    tokens, depth = h.shape
    hidden = gate.shape[1]
    cw = 256 if hidden % 256 == 0 else 128
    chunks = hidden // cw
    k, kc, crows = log2(n), log2(nc), tokens // nc
    vmem = pl.BlockSpec(memory_space=pltpu.VMEM)
    hbm = pl.BlockSpec(memory_space=pl.ANY)
    dma = pltpu.SemaphoreType.DMA
    if first:
        out = [
            jax.ShapeDtypeStruct((tokens, depth), BF16),
            jax.ShapeDtypeStruct((crows, depth), F32),
            jax.ShapeDtypeStruct((nc, 8, crows), F32),
        ]
    else:
        out = [jax.ShapeDtypeStruct((tokens, depth), BF16)]
    scratch = [
        pltpu.VMEM((chunks, depth, 2 * cw), BF16),
        pltpu.VMEM((chunks, cw, depth), BF16),
        pltpu.VMEM((chunks, tokens // 2, 2 * cw), F32),
        pltpu.VMEM((chunks, tokens, cw), BF16),
        pltpu.VMEM((tokens, depth), F32),
        pltpu.VMEM((tokens, 128), F32),
        pltpu.VMEM((n - 1, nc, 8, crows), F32),
        pltpu.VMEM((n - 1, 8, crows), F32),
        pltpu.VMEM((8, crows), F32),
        pltpu.VMEM((tokens, depth), BF16),
        pltpu.VMEM((nc, 8, crows), F32),
    ]
    scratch += [pltpu.VMEM((chunks, tokens >> (s + 1), 2 * cw), BF16) for s in range(k)] * 2
    scratch += [pltpu.VMEM((tokens >> (s + 1), depth), BF16 if s else F32) for s in range(kc)] * 2
    scratch += [dma((3, chunks))] + [dma((k, chunks))] * 4 + [dma((kc,))] * 2
    scratch += [dma((n - 1,))] * 4 + [dma((kc,))] * 2 + [dma((nc - 1,))] * 2
    return pl.pallas_call(
        functools.partial(half_step, first, n, nc, width),
        out_shape=out,
        in_specs=[vmem] * 5 + [hbm] * 3,
        out_specs=[vmem] * len(out),
        scratch_shapes=scratch,
        compiler_params=pltpu.CompilerParams(
            collective_id=0 if first else 1, has_side_effects=True, vmem_limit_bytes=60 * 1024 * 1024
        ),
        name="first" if first else "second",
    )(h, resid, ss, post, pre, gate, up, down)


def solution(mesh):
    n, nc = mesh.shape["ra"], mesh.shape["cb"]

    def body(tokens, pre1, gate1, up1, down1, post1, pre2, gate2, up2, down2, post2):
        count, depth = tokens.shape
        width = depth * n
        resid = tokens.astype(F32)
        squares = jnp.sum(resid * resid, axis=1).reshape(nc, 1, count // nc)
        ss = jnp.broadcast_to(squares, (nc, 8, count // nc))
        h = (resid * pre1[None, :]).astype(BF16)
        row = lambda gain: gain.reshape(1, depth)
        h2, mid, ss2 = run(True, n, nc, width, h, tokens, ss, row(post1), row(pre2), gate1, up1, down1)
        (out,) = run(False, n, nc, width, h2, mid, ss2, row(post2), row(pre2), gate2, up2, down2)
        return out

    in_specs = (
        P(None, "ra"), P("ra"), P("ra", "cb"), P("ra", "cb"), P("cb", "ra"), P("ra"),
        P("ra"), P("ra", "cb"), P("ra", "cb"), P("cb", "ra"), P("ra"),
    )
    return jax.shard_map(body, mesh=mesh, in_specs=in_specs, out_specs=P(None, "ra"), check_vma=False)
```
